32 devices in a mesh: grp: 2 (over y), sp: 4 (over z), tp: 4 (over x, core).
Axes of the slice: x: 2, y: 2, z: 4, core: 2. Of those that a mesh axis runs over, the one named last changes fastest.
Arguments:
- queries: bfloat16 [6144, 1024], P(('grp', 'sp'), 'tp'), parts along dimension 0, may hold values from -8 to 8
- keys: bfloat16 [6144, 256], P(('grp', 'sp')), parts along dimension 0, may hold values from -8 to 8
- values: bfloat16 [6144, 256], P(('grp', 'sp')), parts along dimension 0, may hold values from -6 to 6
- query_gain: float32 [128], replicated, may hold values from 0.2 to 6
- key_gain: float32 [128], replicated, may hold values from 0.2 to 6
- residual: bfloat16 [6144, 2048], P(('grp', 'sp', 'tp')), parts along dimension 0, may hold values from -6 to 6
- out_weight: bfloat16 [1024, 2048], P('tp'), may hold values from -0.1875 to 0.1875
- mix_gain: float32 [2048], replicated, may hold values from 0.1 to 1.9
- ffn_gain: float32 [2048], replicated, may hold values from 0.1 to 1.9
- gate_in: bfloat16 [2048, 5632], P('sp', 'tp'), may hold values from -0.125 to 0.125
- value_in: bfloat16 [2048, 5632], P('sp', 'tp'), may hold values from -0.125 to 0.125
- conv_gate: float32 [3, 5632], P(None, 'tp'), may hold values from -3 to 3
- conv_value: float32 [3, 5632], P(None, 'tp'), may hold values from -3 to 3
- down_t: bfloat16 [2048, 5632], P('sp', 'tp'), may hold values from -0.078125 to 0.078125
Outputs:
- layer_out: bfloat16 [6144, 2048], P(('grp', 'sp', 'tp')), parts along dimension 0
The draws below stay inside these ranges and needn't reach their ends.
There are 2 independent parts, one for each index of `grp`. The reference program is written for one: setup_inputs(seed, part) draws one part's arguments, and reference() takes and returns one part's arrays. A program takes and returns all parts, laid end to end along the dimension named above; an argument that names none is the same for every part. Nothing has to cross between parts.
All inputs are finite; a program needn't handle non-finite values.
Results may differ from the reference program's by a relative error of at most 0.02.
The reference program's roundings to bfloat16 on the way count: a program that leaves them out, or rounds other values in their place, can miss the bound.
Values may be sent and summed in bfloat16 or wider, within the bound.
A program may use at most 128 MiB of HBM per device.

```python
import math
import jax
import jax.numpy as jnp
from jax import lax

D = 2048
HEADS = 8
KVH = 2
HD = 128
FF = 5632
GRID_W = 64
SEQ = 3072
N_TP = 4


def shared_keys(key):
    base = jax.random.normal(jax.random.fold_in(key, 11), (SEQ, KVH * HD), jnp.float32)
    return jnp.clip(base, -8.0, 8.0)


def draw_keys(key, part):
    base = shared_keys(key)
    return base.astype(jnp.bfloat16)


def draw_queries(key, part):
    drawn = jax.random.normal(jax.random.fold_in(key, 13), (SEQ, HEADS * HD), jnp.float32)
    return jnp.clip(drawn, -8.0, 8.0).astype(jnp.bfloat16)


def gain_draw(key):
    return jnp.clip(1.0 + 0.18 * jax.random.normal(key, (HD,), jnp.float32), 0.2, 2.0)


def draw_query_gain(key, part):
    return gain_draw(jax.random.fold_in(key, 21))


def draw_key_gain(key, part):
    return gain_draw(jax.random.fold_in(key, 22))


def shard_levels(own_key, extent, shards, low, top_value):
    factor_of, own = 1.0, jax.random.fold_in(own_key, 6)
    for position, blocks in shards:
        heights = jnp.exp(jax.random.uniform(jax.random.fold_in(own, position), (blocks,), jnp.float32, low / len(shards), top_value / len(shards)))
        factor_of = factor_of * jnp.repeat(heights, extent[position] // blocks).reshape([-1 if axis == position else 1 for axis in range(len(extent))])
    return factor_of


def centred(key, shape, scale, limit, cuts=(), held_as=jnp.bfloat16):
    result = jax.random.normal(key, shape, jnp.float32) * scale
    if len(cuts) > 0:
        result = shard_levels(key, shape, cuts, -0.22, 0.18) * result
    return jnp.clip(result, min=-limit, max=limit).astype(held_as)


def setup_inputs(seed: int = 0, part: int = 0) -> dict:
    arg_keys = jax.random.split(jax.random.key(seed), 15)
    own_keys = jax.random.split(jax.random.fold_in(arg_keys[14], part), 15)
    queries = draw_queries(jax.random.fold_in(jax.random.fold_in(arg_keys[14], part), 71), part)
    keys = draw_keys(jax.random.fold_in(jax.random.fold_in(arg_keys[14], part), 71), part)
    values = centred(own_keys[2], (SEQ, KVH * HD), 1.0, 6.0, ((0, 4),))
    query_gain = draw_query_gain(jax.random.fold_in(arg_keys[14], 71), part)
    key_gain = draw_key_gain(jax.random.fold_in(arg_keys[14], 71), part)
    residual = centred(own_keys[5], (SEQ, D), 1.0, 6.0, ((0, 16),))
    out_weight = centred(arg_keys[6], (HEADS * HD, D), (HEADS * HD) ** -0.5, 0.1875, ((0, 4),))
    mix_gain = jnp.clip(1.0 + 0.18 * jax.random.normal(arg_keys[7], (D,), jnp.float32), 0.1, 1.9)
    ffn_gain = jnp.clip(1.0 + 0.18 * jax.random.normal(arg_keys[8], (D,), jnp.float32), 0.1, 1.9)
    gate_in = centred(arg_keys[9], (D, FF), D ** -0.5, 0.125, ((0, 4), (1, 4)))
    value_in = centred(arg_keys[10], (D, FF), D ** -0.5, 0.125, ((0, 4), (1, 4)))
    conv_gate = centred(arg_keys[11], (3, FF), 0.577, 3.0, ((1, 4),), jnp.float32)
    conv_value = centred(arg_keys[12], (3, FF), 0.577, 3.0, ((1, 4),), jnp.float32)
    down_t = centred(arg_keys[13], (D, FF), FF ** -0.5, 0.078125, ((0, 4), (1, 4)))
    return dict(queries=queries, keys=keys, values=values, query_gain=query_gain, key_gain=key_gain, residual=residual, out_weight=out_weight, mix_gain=mix_gain, ffn_gain=ffn_gain, gate_in=gate_in, value_in=value_in, conv_gate=conv_gate, conv_value=conv_value, down_t=down_t)


EPSILON = 1e-06
THETA = 10000.0

def rotary_tables():
    quarter = HD // 4
    inverse = THETA ** (-(2.0 * jnp.arange(quarter, dtype=jnp.float32)) / (HD // 2))
    positions = jnp.arange(SEQ, dtype=jnp.int32)
    grid_row = (positions // GRID_W - SEQ // GRID_W // 2).astype(jnp.float32)
    grid_col = (positions % GRID_W - GRID_W // 2).astype(jnp.float32)
    row_angle = grid_row[:, None] * inverse[None, :]
    col_angle = grid_col[:, None] * inverse[None, :]
    angle = jnp.concatenate([row_angle, row_angle, col_angle, col_angle], axis=-1)
    return (jnp.cos(angle), jnp.sin(angle))

def rotate_quarters(vector):
    first, second, third, fourth = jnp.split(vector, 4, axis=-1)
    return jnp.concatenate([-second, first, -fourth, third], axis=-1)

def prepare_heads(raw, gain, cos_table, sin_table, factor):
    floats = raw.astype(jnp.float32)
    normed = floats * lax.rsqrt(lax.optimization_barrier(jnp.mean(floats * floats, axis=-1, keepdims=True)) + EPSILON) * gain
    turned = normed * cos_table + rotate_quarters(normed) * sin_table
    return (turned * factor).astype(jnp.bfloat16)

def rms_rows(stream, gain):
    floats = stream.astype(jnp.float32)
    return floats * lax.rsqrt(lax.optimization_barrier(jnp.mean(floats * floats, axis=-1, keepdims=True)) + EPSILON) * gain

def reference(queries, keys, values, query_gain, key_gain, residual, out_weight, mix_gain, ffn_gain, gate_in, value_in, conv_gate, conv_value, down_t):
    group = HEADS // KVH
    cos_table, sin_table = rotary_tables()
    query_rot = prepare_heads(queries.reshape(SEQ, HEADS, HD), query_gain, cos_table[:, None, :], sin_table[:, None, :], HD ** (-0.5))
    key_rot = prepare_heads(keys.reshape(SEQ, KVH, HD), key_gain, cos_table[:, None, :], sin_table[:, None, :], 1.0)
    key_float = key_rot.astype(jnp.float32)
    value_float = values.reshape(SEQ, KVH, HD).astype(jnp.float32)
    block = math.gcd(SEQ, 512)
    query_blocks = query_rot.reshape(SEQ // block, block, KVH, group, HD)

    def attend_block(query_block):
        scores = jnp.einsum('qhgd,khd->hgqk', query_block.astype(jnp.float32), key_float)
        highest = lax.optimization_barrier(jnp.max(scores, axis=-1, keepdims=True))
        weights = jnp.exp(scores - highest)
        denom = lax.optimization_barrier(jnp.sum(weights, axis=-1, keepdims=True))
        rounded = weights.astype(jnp.bfloat16).astype(jnp.float32)
        summed = jnp.einsum('hgqk,khd->qhgd', rounded, value_float)
        denom_t = jnp.transpose(denom, (2, 0, 1, 3))
        return (summed / denom_t).astype(jnp.bfloat16)
    attended = lax.map(attend_block, query_blocks).reshape(SEQ, HEADS * HD)
    head_cols = HEADS * HD // N_TP
    mix = jnp.zeros((SEQ, D), jnp.float32)
    for group_index in range(N_TP):
        lower = group_index * head_cols
        partial_mix = jnp.dot(attended[:, lower:lower + head_cols], out_weight[lower:lower + head_cols], preferred_element_type=jnp.float32).astype(jnp.bfloat16)
        partial_mix = lax.optimization_barrier(partial_mix)
        mix = mix + partial_mix.astype(jnp.float32)
    mix_normed = rms_rows(mix, mix_gain)
    stream = (residual.astype(jnp.float32) + mix_normed).astype(jnp.bfloat16)
    normed = rms_rows(stream, ffn_gain).astype(jnp.bfloat16)
    gate_up = jnp.dot(normed, gate_in, preferred_element_type=jnp.float32).astype(jnp.bfloat16)
    value_up = jnp.dot(normed, value_in, preferred_element_type=jnp.float32).astype(jnp.bfloat16)

    def depthwise(upward, taps):
        padded = jnp.pad(upward.astype(jnp.float32), ((1, 1), (0, 0)))
        return taps[0] * padded[:-2] + taps[1] * padded[1:-1] + taps[2] * padded[2:]
    gate_mixed = depthwise(gate_up, conv_gate)
    value_mixed = depthwise(value_up, conv_value)
    hidden = (jax.nn.gelu(gate_mixed, approximate=True) * value_mixed).astype(jnp.bfloat16)
    unit_cols = FF // N_TP
    ffn_out = jnp.zeros((SEQ, D), jnp.float32)
    for group_index in range(N_TP):
        lower = group_index * unit_cols
        partial_down = jnp.dot(hidden[:, lower:lower + unit_cols], down_t[:, lower:lower + unit_cols].T, preferred_element_type=jnp.float32).astype(jnp.bfloat16)
        partial_down = lax.optimization_barrier(partial_down)
        ffn_out = ffn_out + partial_down.astype(jnp.float32)
    return (stream.astype(jnp.float32) + ffn_out).astype(jnp.bfloat16)
```

```python
import jax
import jax.numpy as jnp
from jax import lax
from jax.sharding import PartitionSpec as P

HEADS = 8
KVH = 2
GRID_W = 64


EPSILON = 1e-06
THETA = 10000.0


def with_halo(block, sides, width):
    for axis, dim in sides:
        count = lax.axis_size(axis)
        forward = [(i, i + 1) for i in range(count - 1)]
        backward = [(target, source) for source, target in forward]
        low = lax.ppermute(
            lax.slice_in_dim(block, block.shape[dim] - width, None, axis=dim), axis, forward
        )
        high = lax.ppermute(lax.slice_in_dim(block, 0, width, axis=dim), axis, backward)
        block = jnp.concatenate([low, block, high], axis=dim)
    return block


def rotary_tables(positions, seq_total, head_dim):
    quarter = head_dim // 4
    inverse = THETA ** (-(2.0 * jnp.arange(quarter, dtype=jnp.float32)) / (head_dim // 2))
    grid_row = (positions // GRID_W - seq_total // GRID_W // 2).astype(jnp.float32)
    grid_col = (positions % GRID_W - GRID_W // 2).astype(jnp.float32)
    row_angle = grid_row[:, None] * inverse[None, :]
    col_angle = grid_col[:, None] * inverse[None, :]
    angle = jnp.concatenate([row_angle, row_angle, col_angle, col_angle], axis=-1)
    return (jnp.cos(angle), jnp.sin(angle))


def rotate_quarters(vector):
    first, second, third, fourth = jnp.split(vector, 4, axis=-1)
    return jnp.concatenate([-second, first, -fourth, third], axis=-1)


def prepare_heads(raw, gain, cos_table, sin_table, factor):
    floats = raw.astype(jnp.float32)
    normed = floats * lax.rsqrt(jnp.mean(floats * floats, axis=-1, keepdims=True) + EPSILON) * gain
    turned = normed * cos_table + rotate_quarters(normed) * sin_table
    return (turned * factor).astype(jnp.bfloat16)


def rms_rows(stream, gain):
    floats = stream.astype(jnp.float32)
    return floats * lax.rsqrt(jnp.mean(floats * floats, axis=-1, keepdims=True) + EPSILON) * gain


def shifted(block, axis, step):
    count = lax.axis_size(axis)
    return lax.ppermute(block, axis, [(i, (i + step) % count) for i in range(count)])


def after(value, *others):
    return lax.optimization_barrier((value, *others))[0]


def own_part(block, axis):
    count = lax.axis_size(axis)
    rows = block.shape[0] // count
    return lax.dynamic_slice_in_dim(block, lax.axis_index(axis) * rows, rows, 0)


def ring_step(part):
    return shifted(part, "sp", 1)


def exchanged(part):
    pieces = [part] + [shifted(part, "grp", j) for j in range(1, lax.axis_size("grp"))]
    return pieces


def arrival_columns(array):
    blocks, parts = lax.axis_size("sp"), lax.axis_size("grp")
    me, copy = lax.axis_index("sp"), lax.axis_index("grp")
    width = array.shape[1] // (blocks * parts)
    pieces = []
    for d in range(blocks):
        for j in range(parts):
            place = lax.rem(me - d + blocks, blocks) * parts + lax.rem(copy - j + parts, parts)
            pieces.append(lax.dynamic_slice_in_dim(array, place * width, width, 1))
    return jnp.concatenate(pieces, axis=1)


def own_pieces(block):
    parts = lax.axis_size("grp")
    rows = block.shape[0] // parts
    copy = lax.axis_index("grp")
    return [
        lax.dynamic_slice_in_dim(block, lax.rem(copy - j + parts, parts) * rows, rows, 0)
        for j in range(parts)
    ]


def gathered_kv(kv, pair_shares):
    count = lax.axis_size("sp")
    if not pair_shares:
        return jnp.concatenate([kv] + [shifted(kv, "sp", d) for d in range(1, count)], axis=0)
    tp_count = lax.axis_size("tp")
    rows = kv.shape[0] // 2
    mine = lax.dynamic_slice_in_dim(kv, lax.axis_index("tp") % 2 * rows, rows, 0)
    far = jnp.concatenate([shifted(mine, "sp", d) for d in range(1, count)], axis=0)
    near = lax.ppermute(far, "tp", [(i, i ^ 1) for i in range(tp_count)])
    return jnp.concatenate([kv, far, near], axis=0)


def body(
    queries,
    keys,
    values,
    query_gain,
    key_gain,
    residual,
    out_weight,
    mix_gain,
    ffn_gain,
    gate_in,
    value_in,
    conv_gate,
    conv_value,
    down_t,
):
    blocks, group_count = lax.axis_size("sp"), lax.axis_size("tp")
    whole_out = lax.all_gather(out_weight, "tp", axis=0, tiled=True)
    tok_rows = queries.shape[0]
    head_dim = query_gain.shape[0]
    local_heads = queries.shape[1] // head_dim
    seq_total = tok_rows * blocks
    kv_head = lax.axis_index("tp") * local_heads // (HEADS // KVH)
    positions = lax.axis_index("sp") * tok_rows + jnp.arange(tok_rows, dtype=jnp.int32)
    cos_table, sin_table = rotary_tables(positions, seq_total, head_dim)
    key_own = lax.dynamic_slice_in_dim(keys, kv_head * head_dim, head_dim, 1)
    value_own = lax.dynamic_slice_in_dim(values, kv_head * head_dim, head_dim, 1)
    key_rot = prepare_heads(key_own, key_gain, cos_table, sin_table, 1.0)
    kv_own = jnp.concatenate([key_rot, value_own], axis=1)
    pair_shares = group_count % 2 == 0 and (HEADS // KVH) % (2 * local_heads) == 0
    kv_all = gathered_kv(kv_own, pair_shares)

    gates, vals, downs = [own_pieces(gate_in)], [own_pieces(value_in)], [own_pieces(down_t)]
    gate_part, value_part, down_part = gates[0][0], vals[0][0], downs[0][0]
    gate_part, value_part = lax.optimization_barrier((gate_part, value_part, kv_own))[:2]
    for d in range(1, blocks):
        gate_part = ring_step(gate_part)
        value_part = ring_step(value_part)
        gates.append(exchanged(gate_part))
        vals.append(exchanged(value_part))
        if d == max(blocks - 2, 1):
            down_part = after(down_part, gate_part)
    for d in range(1, blocks):
        down_part = ring_step(down_part)
        downs.append(exchanged(down_part))

    query_rot = prepare_heads(
        queries.reshape(tok_rows, local_heads, head_dim),
        query_gain,
        cos_table[:, None, :],
        sin_table[:, None, :],
        head_dim ** (-0.5),
    )
    query_rows = jnp.transpose(query_rot, (1, 0, 2)).reshape(local_heads * tok_rows, head_dim)
    scores = lax.dot_general(
        query_rows,
        kv_all[:, :head_dim],
        (((1,), (1,)), ((), ())),
        preferred_element_type=jnp.float32,
    )
    newest = jnp.max(scores, axis=1, keepdims=True)
    weights = jnp.exp(scores - newest)
    denom = jnp.sum(weights, axis=1, keepdims=True)
    summed = jnp.dot(
        weights.astype(jnp.bfloat16), kv_all[:, head_dim:], preferred_element_type=jnp.float32
    )
    attended = (summed / denom).astype(jnp.bfloat16).reshape(local_heads, tok_rows, head_dim)
    attended = jnp.transpose(attended, (1, 0, 2)).reshape(tok_rows, local_heads * head_dim)
    own_rows = residual.shape[0]
    token_heads = lax.all_to_all(attended, "tp", split_axis=0, concat_axis=1, tiled=True)
    group_cols = attended.shape[1]
    grouped_rows = token_heads.reshape(own_rows, group_count, group_cols)
    grouped_weight = whole_out.reshape(group_count, group_cols, whole_out.shape[1])
    partials = jnp.einsum(
        "rgc,gcd->grd", grouped_rows, grouped_weight, preferred_element_type=jnp.float32
    ).astype(jnp.bfloat16)
    mix = jnp.sum(partials.astype(jnp.float32), axis=0)
    stream = (residual.astype(jnp.float32) + rms_rows(mix, mix_gain)).astype(jnp.bfloat16)
    normed = rms_rows(stream, ffn_gain).astype(jnp.bfloat16)
    all_normed = lax.all_gather(arrival_columns(normed), "tp", axis=0, tiled=True)

    def up(pieces):
        rows = jnp.concatenate([piece for block in pieces for piece in block], axis=0)
        return jnp.dot(all_normed, rows, preferred_element_type=jnp.float32).astype(jnp.bfloat16)

    upward = jnp.concatenate([up(gates), up(vals)], axis=1)
    padded = with_halo(upward, (("sp", 0),), 1).astype(jnp.float32)
    taps = jnp.concatenate([conv_gate, conv_value], axis=1)
    mixed = taps[0] * padded[:-2] + taps[1] * padded[1:-1] + taps[2] * padded[2:]
    unit_cols = conv_gate.shape[1]
    hidden = (jax.nn.gelu(mixed[:, :unit_cols], approximate=True) * mixed[:, unit_cols:]).astype(
        jnp.bfloat16
    )
    shares = []
    for block in downs:
        rows = jnp.concatenate(block, axis=0)
        partial = lax.dot_general(
            hidden, rows, (((1,), (1,)), ((), ())), preferred_element_type=jnp.float32
        ).astype(jnp.bfloat16)
        shares.append(lax.psum_scatter(partial, "tp", scatter_dimension=0, tiled=True))
    ffn_out = arrival_columns(jnp.concatenate(shares, axis=1)).astype(jnp.float32)
    return (stream.astype(jnp.float32) + ffn_out).astype(jnp.bfloat16)


def solution(mesh):
    return jax.shard_map(
        body,
        mesh=mesh,
        in_specs=(
            P(("grp", "sp"), "tp"),
            P(("grp", "sp"), None),
            P(("grp", "sp"), None),
            P(),
            P(),
            P(("grp", "sp", "tp"), None),
            P("tp", None),
            P(),
            P(),
            P("sp", "tp"),
            P("sp", "tp"),
            P(None, "tp"),
            P(None, "tp"),
            P("sp", "tp"),
        ),
        out_specs=P(("grp", "sp", "tp"), None),
        check_vma=False,
    )
```

```python
import jax
import jax.numpy as jnp
from jax import lax
from jax.sharding import PartitionSpec as P


HEADS = 8
KVH = 2
GRID_W = 64


EPSILON = 1e-06
THETA = 10000.0


def with_halo(block, sides, width):
    for axis, dim in sides:
        count = lax.axis_size(axis)
        forward = [(i, i + 1) for i in range(count - 1)]
        backward = [(target, source) for source, target in forward]
        low = lax.ppermute(
            lax.slice_in_dim(block, block.shape[dim] - width, None, axis=dim), axis, forward
        )
        high = lax.ppermute(lax.slice_in_dim(block, 0, width, axis=dim), axis, backward)
        block = jnp.concatenate([low, block, high], axis=dim)
    return block


def rotary_tables(positions, seq_total, head_dim):
    quarter = head_dim // 4
    inverse = THETA ** (-(2.0 * jnp.arange(quarter, dtype=jnp.float32)) / (head_dim // 2))
    grid_row = (positions // GRID_W - seq_total // GRID_W // 2).astype(jnp.float32)
    grid_col = (positions % GRID_W - GRID_W // 2).astype(jnp.float32)
    row_angle = grid_row[:, None] * inverse[None, :]
    col_angle = grid_col[:, None] * inverse[None, :]
    angle = jnp.concatenate([row_angle, row_angle, col_angle, col_angle], axis=-1)
    return (jnp.cos(angle), jnp.sin(angle))


def rotate_quarters(vector):
    first, second, third, fourth = jnp.split(vector, 4, axis=-1)
    return jnp.concatenate([-second, first, -fourth, third], axis=-1)


def prepare_heads(raw, gain, cos_table, sin_table, factor):
    floats = raw.astype(jnp.float32)
    normed = floats * lax.rsqrt(jnp.mean(floats * floats, axis=-1, keepdims=True) + EPSILON) * gain
    turned = normed * cos_table + rotate_quarters(normed) * sin_table
    return (turned * factor).astype(jnp.bfloat16)


def rms_rows(stream, gain):
    floats = stream.astype(jnp.float32)
    return floats * lax.rsqrt(jnp.mean(floats * floats, axis=-1, keepdims=True) + EPSILON) * gain


def shifted(block, axis, step):
    count = lax.axis_size(axis)
    return lax.ppermute(block, axis, [(i, (i + step) % count) for i in range(count)])


def after(value, *others):
    return lax.optimization_barrier((value, *others))[0]


def ring_step(part):
    return shifted(part, "sp", 1)


def exchanged(part):
    pieces = [part] + [shifted(part, "grp", j) for j in range(1, lax.axis_size("grp"))]
    return pieces


def arrival_places(d):
    blocks, parts = lax.axis_size("sp"), lax.axis_size("grp")
    block = lax.rem(lax.axis_index("sp") - d + blocks, blocks)
    copy = lax.axis_index("grp")
    return [block * parts + lax.rem(copy - j + parts, parts) for j in range(parts)]


def arrival_columns(array):
    blocks, parts = lax.axis_size("sp"), lax.axis_size("grp")
    width = array.shape[1] // (blocks * parts)
    places = [place for d in range(blocks) for place in arrival_places(d)]
    return jnp.concatenate(
        [lax.dynamic_slice_in_dim(array, place * width, width, 1) for place in places], axis=1
    )


def own_pieces(block):
    parts = lax.axis_size("grp")
    rows = block.shape[0] // parts
    copy = lax.axis_index("grp")
    return [
        lax.dynamic_slice_in_dim(block, lax.rem(copy - j + parts, parts) * rows, rows, 0)
        for j in range(parts)
    ]


def gathered_kv(kv, pair_shares):
    count = lax.axis_size("sp")
    if not pair_shares:
        return jnp.concatenate([kv] + [shifted(kv, "sp", d) for d in range(1, count)], axis=0)
    tp_count = lax.axis_size("tp")
    rows = kv.shape[0] // 2
    mine = lax.dynamic_slice_in_dim(kv, lax.axis_index("tp") % 2 * rows, rows, 0)
    far = jnp.concatenate([shifted(mine, "sp", d) for d in range(1, count)], axis=0)
    near = lax.ppermute(far, "tp", [(i, i ^ 1) for i in range(tp_count)])
    return jnp.concatenate([kv, far, near], axis=0)


def body(
    queries,
    keys,
    values,
    query_gain,
    key_gain,
    residual,
    out_weight,
    mix_gain,
    ffn_gain,
    gate_in,
    value_in,
    conv_gate,
    conv_value,
    down_t,
):
    blocks, group_count = lax.axis_size("sp"), lax.axis_size("tp")
    whole_out = lax.all_gather(out_weight, "tp", axis=0, tiled=True)
    tok_rows = queries.shape[0]
    head_dim = query_gain.shape[0]
    local_heads = queries.shape[1] // head_dim
    seq_total = tok_rows * blocks
    kv_head = lax.axis_index("tp") * local_heads // (HEADS // KVH)
    positions = lax.axis_index("sp") * tok_rows + jnp.arange(tok_rows, dtype=jnp.int32)
    cos_table, sin_table = rotary_tables(positions, seq_total, head_dim)
    key_own = lax.dynamic_slice_in_dim(keys, kv_head * head_dim, head_dim, 1)
    value_own = lax.dynamic_slice_in_dim(values, kv_head * head_dim, head_dim, 1)
    key_rot = prepare_heads(key_own, key_gain, cos_table, sin_table, 1.0)
    kv_own = jnp.concatenate([key_rot, value_own], axis=1)
    pair_shares = group_count % 2 == 0 and (HEADS // KVH) % (2 * local_heads) == 0
    kv_all = gathered_kv(kv_own, pair_shares)

    gates, vals, downs = [own_pieces(gate_in)], [own_pieces(value_in)], [own_pieces(down_t)]
    gate_part, value_part, down_part = gates[0][0], vals[0][0], downs[0][0]
    gate_steps, value_steps, down_steps = [gate_part], [value_part], [down_part]
    for _ in range(1, blocks):
        gate_part = ring_step(gate_part)
        value_part = ring_step(value_part)
        gates.append(exchanged(gate_part))
        vals.append(exchanged(value_part))
        gate_steps.append(gate_part)
        value_steps.append(value_part)
    down_part = after(down_part, gate_part)
    for _ in range(1, blocks - 1):
        down_part = ring_step(down_part)
        downs.append(exchanged(down_part))
        down_steps.append(down_part)
    last = []
    for half in jnp.split(down_part, 2, axis=0):
        half = ring_step(half)
        last.append(exchanged(half))

    query_rot = prepare_heads(
        queries.reshape(tok_rows, local_heads, head_dim),
        query_gain,
        cos_table[:, None, :],
        sin_table[:, None, :],
        head_dim ** (-0.5),
    )
    query_rows = jnp.transpose(query_rot, (1, 0, 2)).reshape(local_heads * tok_rows, head_dim)
    scores = lax.dot_general(
        query_rows,
        kv_all[:, :head_dim],
        (((1,), (1,)), ((), ())),
        preferred_element_type=jnp.float32,
    )
    newest = jnp.max(scores, axis=1, keepdims=True)
    step_one, step_two = min(1, blocks - 1), min(2, blocks - 1)
    down_one, down_two = min(1, len(down_steps) - 1), min(2, len(down_steps) - 1)
    scores, newest, _ = lax.optimization_barrier((scores, newest, gate_steps[step_one]))
    weights = jnp.exp(scores - newest)
    denom = jnp.sum(weights, axis=1, keepdims=True)
    value_all = after(kv_all[:, head_dim:], value_steps[step_one], denom)
    summed = jnp.dot(weights.astype(jnp.bfloat16), value_all, preferred_element_type=jnp.float32)
    attended = (summed / denom).astype(jnp.bfloat16).reshape(local_heads, tok_rows, head_dim)
    attended = jnp.transpose(attended, (1, 0, 2)).reshape(tok_rows, local_heads * head_dim)
    own_rows = residual.shape[0]
    token_heads = lax.all_to_all(attended, "tp", split_axis=0, concat_axis=1, tiled=True)
    token_heads = after(token_heads, gate_steps[step_two])
    group_cols = attended.shape[1]
    grouped_rows = token_heads.reshape(own_rows, group_count, group_cols)
    grouped_weight = whole_out.reshape(group_count, group_cols, whole_out.shape[1])
    partials = jnp.einsum(
        "rgc,gcd->grd", grouped_rows, grouped_weight, preferred_element_type=jnp.float32
    ).astype(jnp.bfloat16)
    mix = jnp.sum(partials.astype(jnp.float32), axis=0)
    stream = (residual.astype(jnp.float32) + rms_rows(mix, mix_gain)).astype(jnp.bfloat16)
    normed = rms_rows(stream, ffn_gain).astype(jnp.bfloat16)
    columns = arrival_columns(normed)
    all_normed = lax.all_gather(columns, "tp", axis=0, tiled=True)
    all_normed = after(all_normed, down_steps[down_one])

    def up(pieces):
        rows = jnp.concatenate([piece for block in pieces for piece in block], axis=0)
        return jnp.dot(all_normed, rows, preferred_element_type=jnp.float32).astype(jnp.bfloat16)

    up_gate = up(gates)
    up_value = up(vals)
    upward = jnp.concatenate([up_gate, up_value], axis=1)
    upward = after(upward, down_steps[down_two])
    padded = with_halo(upward, (("sp", 0),), 1).astype(jnp.float32)
    taps = jnp.concatenate([conv_gate, conv_value], axis=1)
    mixed = taps[0] * padded[:-2] + taps[1] * padded[1:-1] + taps[2] * padded[2:]
    unit_cols = conv_gate.shape[1]
    hidden = (jax.nn.gelu(mixed[:, :unit_cols], approximate=True) * mixed[:, unit_cols:]).astype(
        jnp.bfloat16
    )
    out = jnp.zeros_like(stream)
    arrivals = [(d, 0, block) for d, block in enumerate(downs)]
    arrivals += [(blocks - 1, h, block) for h, block in enumerate(last)]
    groups = [arrivals[:2]] + [[arrival] for arrival in arrivals[2:]]
    stride = down_part.shape[0]
    for group in groups:
        rows = jnp.concatenate([part for _, _, block in group for part in block], axis=0)
        partial = lax.dot_general(
            hidden, rows, (((1,), (1,)), ((), ())), preferred_element_type=jnp.float32
        ).astype(jnp.bfloat16)
        shares = lax.all_to_all(
            partial.reshape(group_count, own_rows, rows.shape[0]), "tp", 0, 0, tiled=True
        )
        added = jnp.sum(shares.astype(jnp.float32), axis=0)
        places = [
            (place * stride + h * block[0].shape[0], block[0].shape[0])
            for d, h, block in group
            for place in arrival_places(d)
        ]
        begin = 0
        for first, width in places:
            piece = lax.dynamic_slice_in_dim(stream, first, width, 1).astype(jnp.float32)
            piece = (piece + added[:, begin : begin + width]).astype(jnp.bfloat16)
            out = lax.dynamic_update_slice_in_dim(out, piece, first, 1)
            begin += width
    return out


def solution(mesh):
    return jax.shard_map(
        body,
        mesh=mesh,
        in_specs=(
            P(("grp", "sp"), "tp"),
            P(("grp", "sp"), None),
            P(("grp", "sp"), None),
            P(),
            P(),
            P(("grp", "sp", "tp"), None),
            P("tp", None),
            P(),
            P(),
            P("sp", "tp"),
            P("sp", "tp"),
            P(None, "tp"),
            P(None, "tp"),
            P("sp", "tp"),
        ),
        out_specs=P(("grp", "sp", "tp"), None),
        check_vma=False,
    )
```
